32 devices in a mesh: sp: 8 (over z, x), tp: 4 (over y, core).
Axes of the slice: x: 2, y: 2, z: 4, core: 2. Of those that a mesh axis runs over, the one named last changes fastest.
Arguments:
- tokens: bfloat16 [2048, 2048], P('sp', 'tp'), may hold values from -6 to 6
- norm_gain: float32 [2048], replicated, may hold values from 0.1 to 1.9
- query_one: bfloat16 [2048, 512], P('sp', 'tp'), may hold values from -1 to 1
- key_one: bfloat16 [2048, 512], P('sp', 'tp'), may hold values from -1 to 1
- query_two: bfloat16 [2048, 512], P('sp', 'tp'), may hold values from -0.15625 to 0.15625
- key_two: bfloat16 [2048, 512], P('sp', 'tp'), may hold values from -0.15625 to 0.15625
- value_weight: bfloat16 [2048, 1024], P('sp', 'tp'), may hold values from -0.5 to 0.5
- pool_weight: bfloat16 [2048, 1024], P('sp', 'tp'), may hold values from -0.125 to 0.125
- lambda_head: float32 [8], replicated, may hold values from 0.3 to 0.8
- head_gain: float32 [128], replicated, may hold values from 0.1 to 1.9
- group_weight: bfloat16 [8, 128, 128], replicated, may hold values from -0.5 to 0.5
- pool_scale: float32 [1024], replicated, may hold values from 0.1 to 1.9
- out_attn: bfloat16 [1024, 2048], P('tp', 'sp'), may hold values from -0.125 to 0.125
- out_pool: bfloat16 [1024, 2048], P('tp', 'sp'), may hold values from -0.125 to 0.125
Outputs:
- mixed: bfloat16 [2048, 2048], P(('sp', 'tp'))
The draws below stay inside these ranges and needn't reach their ends.
All inputs are finite; a program needn't handle non-finite values.
Results may differ from the reference program's by a relative error of at most 0.013.
Values may be sent and summed in bfloat16 or wider, within the bound.
No kernel may reach another device: no remote copies, remote signals or barrier semaphores. Data moves between devices by JAX's collectives and lax.ppermute only.
A program may use at most 128 MiB of HBM per device.

```python
import math
import jax
import jax.numpy as jnp
from jax import lax

D = 2048
HEADS = 8
HEAD_DIM = 64
VALUE_DIM = 128
GROUPS = 8
GROUP_DIM = 128
TOKENS = 2048


def paired_weights(key):
    first_draw = jax.random.normal(jax.random.fold_in(key, 101), (D, HEADS * HEAD_DIM), jnp.float32)
    second_draw = jax.random.normal(jax.random.fold_in(key, 202), (D, HEADS * HEAD_DIM), jnp.float32)
    query_part = jnp.clip(first_draw, -4.0, 4.0) * (1.3 / jnp.sqrt(jnp.float32(D)))
    key_part = jnp.clip(second_draw, -4.0, 4.0) * (1.3 / jnp.sqrt(jnp.float32(D)))
    return (query_part, key_part)


def draw_query_one(key, part):
    return paired_weights(key)[0].astype(jnp.bfloat16)


def draw_key_one(key, part):
    return paired_weights(key)[1].astype(jnp.bfloat16)


def levels(rng, shape, shards, smallest, high):
    gain = 1.0
    for position, blocks in shards:
        steps = jax.random.uniform(jax.random.fold_in(jax.random.fold_in(rng, 6), position), (blocks,), jnp.float32, smallest / len(shards), high / len(shards))
        gain = gain * jnp.repeat(jnp.exp(steps), shape[position] // blocks).reshape((-1,) + (1,) * (len(shape) - 1 - position))
    return gain


def normal_values(key, extent, spread, limit, split=(), held_as=jnp.bfloat16):
    loudness = levels(key, extent, split, -0.22, 0.18) if split else 1.0
    array = jax.random.normal(key, extent, jnp.float32) * spread * loudness
    return jnp.minimum(jnp.maximum(array, -limit), limit).astype(held_as)


def setup_inputs(seed: int = 0) -> dict:
    arg_keys = jax.random.split(jax.random.key(seed), 15)
    return {
        "tokens": normal_values(arg_keys[0], (TOKENS, D), 1.0, 6.0, ((0, 8), (1, 4))),
        "norm_gain": jnp.clip(1.0 + 0.18 * jax.random.normal(arg_keys[1], (D,), jnp.float32), 0.1, 1.9),
        "query_one": draw_query_one(jax.random.fold_in(arg_keys[14], 71), 0),
        "key_one": draw_key_one(jax.random.fold_in(arg_keys[14], 71), 0),
        "query_two": normal_values(arg_keys[4], (D, HEADS * HEAD_DIM), (D * 100 // 169) ** -0.5, 0.15625, ((0, 8), (1, 4))),
        "key_two": normal_values(arg_keys[5], (D, HEADS * HEAD_DIM), (D * 100 // 169) ** -0.5, 0.15625, ((0, 8), (1, 4))),
        "value_weight": normal_values(arg_keys[6], (D, HEADS * VALUE_DIM), (D // 16) ** -0.5, 0.5, ((0, 8), (1, 4))),
        "pool_weight": normal_values(arg_keys[7], (D, GROUPS * GROUP_DIM), D ** -0.5, 0.125, ((0, 8), (1, 4))),
        "lambda_head": jnp.clip(jax.random.uniform(arg_keys[8], (HEADS,), jnp.float32, 0.3, 0.8), 0.3, 0.8),
        "head_gain": jnp.clip(1.0 + 0.18 * jax.random.normal(arg_keys[9], (VALUE_DIM,), jnp.float32), 0.1, 1.9),
        "group_weight": normal_values(arg_keys[10], (GROUPS, GROUP_DIM, GROUP_DIM), GROUP_DIM ** -0.5, 0.5),
        "pool_scale": jnp.clip(1.0 + 0.18 * jax.random.normal(arg_keys[11], (GROUPS * GROUP_DIM,), jnp.float32), 0.1, 1.9),
        "out_attn": normal_values(arg_keys[12], (HEADS * VALUE_DIM, D), (HEADS * VALUE_DIM + GROUPS * GROUP_DIM) ** -0.5, 0.125, ((0, 4), (1, 8))),
        "out_pool": normal_values(arg_keys[13], (GROUPS * GROUP_DIM, D), (HEADS * VALUE_DIM + GROUPS * GROUP_DIM) ** -0.5, 0.125, ((0, 4), (1, 8))),
    }


rope_base = 500000.0
head_scale = 0.8
norm_floor = 1e-06
head_floor = 0.001
masked_score = -1e+30

def rotate(values_in, positions):
    half_dim = values_in.shape[-1] // 2
    inverse = rope_base ** (-(jnp.arange(half_dim, dtype=jnp.float32) * 2.0 / values_in.shape[-1]))
    angles = positions.astype(jnp.float32)[:, None] * inverse[None, :]
    cosine = jnp.cos(angles)[:, None, :]
    sine_part = jnp.sin(angles)[:, None, :]
    first_half = values_in[..., :half_dim]
    second_half = values_in[..., half_dim:]
    return jnp.concatenate([first_half * cosine - second_half * sine_part, second_half * cosine + first_half * sine_part], axis=-1)

def reference(tokens, norm_gain, query_one, key_one, query_two, key_two, value_weight, pool_weight, lambda_head, head_gain, group_weight, pool_scale, out_attn, out_pool):
    float_rows = tokens.astype(jnp.float32)
    normed = (float_rows * lax.rsqrt(lax.optimization_barrier(jnp.mean(float_rows * float_rows, axis=-1, keepdims=True)) + norm_floor) * norm_gain).astype(jnp.bfloat16)
    positions = jnp.arange(TOKENS, dtype=jnp.int32)
    score_scale = HEAD_DIM ** (-0.5)

    def project(weight):
        return jnp.dot(normed, weight, preferred_element_type=jnp.float32)

    def turned(weight):
        rounded_rows = rotate(project(weight).reshape(TOKENS, HEADS, HEAD_DIM), positions).astype(jnp.bfloat16)
        return lax.optimization_barrier(rounded_rows).astype(jnp.float32)
    query_a = turned(query_one)
    key_a = turned(key_one)
    query_b = turned(query_two)
    key_b = turned(key_two)
    value_rows = lax.optimization_barrier(project(value_weight).astype(jnp.bfloat16)).astype(jnp.float32).reshape(TOKENS, HEADS, VALUE_DIM)
    query_block = math.gcd(TOKENS, 256)
    blocks = TOKENS // query_block

    def one_block(block_id):
        start_row = block_id * query_block
        query_pos = start_row + jnp.arange(query_block, dtype=jnp.int32)
        visible = (positions[None, :] <= query_pos[:, None])[:, None, :]
        map_means = []
        for query_all, key_all in ((query_a, key_a), (query_b, key_b)):
            query_part = lax.dynamic_slice_in_dim(query_all, start_row, query_block, 0)
            scores = jnp.einsum('qhd,khd->qhk', query_part, key_all) * score_scale
            scores = jnp.where(visible, scores, masked_score)
            top_row = lax.optimization_barrier(jnp.max(scores, axis=-1, keepdims=True))
            weights = jnp.where(visible, jnp.exp(scores - top_row), 0.0)
            totals = lax.optimization_barrier(jnp.sum(weights, axis=-1))
            rounded = lax.optimization_barrier(weights.astype(jnp.bfloat16)).astype(jnp.float32)
            map_means.append(jnp.einsum('qhk,khd->qhd', rounded, value_rows) / totals[..., None])
        differed = map_means[0] - lambda_head[None, :, None] * map_means[1]
        scaled = differed * lax.rsqrt(lax.optimization_barrier(jnp.mean(differed * differed, axis=-1, keepdims=True)) + head_floor) * head_gain * head_scale
        return scaled.astype(jnp.bfloat16)
    attn_out = lax.map(one_block, jnp.arange(blocks, dtype=jnp.int32)).reshape(TOKENS, HEADS * VALUE_DIM)
    pool_rows = lax.optimization_barrier(project(pool_weight).astype(jnp.bfloat16)).astype(jnp.float32)
    running = jnp.cumsum(pool_rows, axis=0)
    results = []
    for group_id in range(GROUPS):
        window = 2 ** (group_id % 4 + 1)
        first_col = group_id * GROUP_DIM
        section = running[:, first_col:first_col + GROUP_DIM]
        earlier = jnp.pad(section, ((window, 0), (0, 0)))[:TOKENS]
        counts = jnp.minimum(positions + 1, window).astype(jnp.float32)
        window_mean = (section - earlier) / counts[:, None] - pool_rows[:, first_col:first_col + GROUP_DIM]
        results.append(jnp.dot(window_mean.astype(jnp.bfloat16), group_weight[group_id], preferred_element_type=jnp.float32))
    pooled = (jnp.concatenate(results, axis=1) * pool_scale).astype(jnp.bfloat16)
    mixed = jnp.dot(attn_out, out_attn, preferred_element_type=jnp.float32) + jnp.dot(pooled, out_pool, preferred_element_type=jnp.float32)
    return mixed.astype(jnp.bfloat16)
```

```python
import jax
import jax.numpy as jnp
from jax import lax
from jax.experimental import pallas as pl
from jax.experimental.pallas import tpu as pltpu
from jax.sharding import PartitionSpec as P

HEAD_DIM = 64
VALUE_DIM = 128
GROUP_DIM = 128
HALO = 16

rope_base = 500000.0
head_scale = 0.8
norm_floor = 1e-06
head_floor = 0.001
masked_score = -1e30

X = 1
HB = 2
Y = 2
C = 1


VMEM = pl.BlockSpec(memory_space=pltpu.VMEM)
SMEM = pl.BlockSpec(memory_space=pltpu.SMEM)


def call(kernel, outs, args, scratch=(), name=None, flops=0):
    return pl.pallas_call(
        kernel,
        out_shape=outs,
        in_specs=[SMEM] + [VMEM] * (len(args) - 1),
        out_specs=jax.tree.map(lambda _: VMEM, outs),
        scratch_shapes=scratch,
        name=name,
        compiler_params=pltpu.CompilerParams(vmem_limit_bytes=48 * 1024 * 1024),
    )(*args)


def pack_kernel(info, q1, k1, q2, k2, v, pool, same, other):
    odd = (info[0] // HB) % 2 == 1
    half = HEAD_DIM

    def pick(j):
        cut = slice(j * half, (j + 1) * half)
        wide = slice(j * VALUE_DIM, (j + 1) * VALUE_DIM)
        return jnp.concatenate(
            [q1[:, cut], q2[:, cut], k1[:, cut], k2[:, cut], v[:, wide], pool[:, wide]], axis=1
        )

    first, second = pick(0), pick(1)
    same[...] = jnp.where(odd, second, first)
    other[...] = jnp.where(odd, first, second)


def pack_out_kernel(info, attn, pool, same, other):
    odd = (info[0] // HB) % 2 == 1
    n = VALUE_DIM
    for at, rows in ((0, attn), (n, pool)):
        first, second = rows[:n, :], rows[n:, :]
        same[at : at + n, :] = jnp.where(odd, second, first)
        other[at : at + n, :] = jnp.where(odd, first, second)


def norm_kernel(info, gain, *refs):
    pieces, out = refs[:-1], refs[-1]
    s, t = info[0], info[1]
    rows, feats = pieces[0].shape
    depth = out.shape[1]
    low = (s // HB) % 2
    for kz in range(2):
        parts = [pieces[kz * 4 + k][...].astype(jnp.float32) for k in range(4)]
        total = sum(jnp.sum(p * p, axis=-1, keepdims=True) for p in parts)
        scale = lax.rsqrt(total / depth + norm_floor)
        at = pl.multiple_of((low ^ kz) * rows, rows)
        for k in range(4):
            col = pl.multiple_of((t ^ k) * feats, feats)
            piece = parts[k] * scale * gain[:, pl.ds(col, feats)]
            out[pl.ds(at, rows), pl.ds(col, feats)] = piece.astype(jnp.bfloat16)


def project_kernel(rels, info, normed, cosine, sine, *refs):
    n = len(rels)
    pieces, (query, keyval, pool, weight) = refs[:n], refs[n:]
    s = info[0]
    deep = pieces[0].shape[0]
    for r, piece in zip(rels, pieces):
        at = pl.multiple_of((s ^ r) * deep, deep)
        weight[pl.ds(at, deep), :] = piece[...]
    made = jnp.dot(normed[...], weight[...], preferred_element_type=jnp.float32)
    rows = made.shape[0]
    lane = lax.broadcasted_iota(jnp.int32, (rows, 2 * HEAD_DIM), 1)
    lower = lane % HEAD_DIM < HEAD_DIM // 2
    quarter = HEAD_DIM // 2

    def turned(x):
        swapped = jnp.where(
            lower,
            pltpu.roll(x, 2 * HEAD_DIM - quarter, 1),
            pltpu.roll(x, quarter, 1),
        )
        return (x * cosine[...] + swapped * sine[...]).astype(jnp.bfloat16)

    w = VALUE_DIM
    query[...] = turned(made[:, :w]) * jnp.bfloat16(HEAD_DIM**-0.5)
    keyval[:rows, :w] = turned(made[:, w : 2 * w])
    keyval[:rows, w:] = made[:, 2 * w : 3 * w].astype(jnp.bfloat16)
    pooled = made[:, 3 * w :].astype(jnp.bfloat16)
    pool[...] = pooled
    half = rows // 2
    keyval[rows:, :w] = pooled[half - HALO : half, :]
    keyval[rows:, w:] = pooled[rows - HALO :, :]


def attend(rels, s, query, pieces, state):
    rows = query.shape[0]
    half = rows // 2
    base = s - ((s // HB) % 2) * HB
    lane = lax.broadcasted_iota(jnp.int32, (half, 2 * HEAD_DIM), 1)
    for r, piece in zip(rels, pieces):
        key_base = base ^ r
        for i in range(2):
            begin = (base + i * HB) * half
            key_begin = key_base * half
            key_last = (key_base + HB) * half + half - 1
            span = slice(i * half, (i + 1) * half)

            def block(masked, piece=piece, begin=begin, key_base=key_base, span=span, first=r == 0):
                asked = query[span, :]
                keys, values = piece[:rows, :VALUE_DIM], piece[:rows, VALUE_DIM:]
                if masked:
                    key_at = lax.broadcasted_iota(jnp.int32, (half, rows), 1)
                    key_at = key_base * half + key_at + jnp.where(key_at >= half, HB * half - half, 0)
                    at = begin + lax.broadcasted_iota(jnp.int32, (half, rows), 0)
                    visible = key_at <= at
                for m in range(2):
                    mine = jnp.where((lane < HEAD_DIM) == (m == 0), asked, jnp.bfloat16(0))
                    scores = lax.dot_general(
                        mine, keys, (((1,), (1,)), ((), ())), preferred_element_type=jnp.float32
                    )
                    if masked:
                        scores = jnp.where(visible, scores, masked_score)
                    top = jnp.max(scores, axis=-1, keepdims=True)
                    if not first:
                        old = state[m, 0, span, :][:, :1]
                        top = jnp.maximum(old, top)
                    weights = jnp.exp(scores - top)
                    total = jnp.sum(weights, axis=-1, keepdims=True)
                    mean = jnp.dot(
                        weights.astype(jnp.bfloat16), values, preferred_element_type=jnp.float32
                    )
                    if not first:
                        factor = jnp.exp(old - top)
                        total = total + state[m, 1, span, :][:, :1] * factor
                        mean = mean + state[m, 2, span, :] * factor
                    shape = (half, VALUE_DIM)
                    state[m, 0, span, :] = jnp.broadcast_to(top, shape)
                    state[m, 1, span, :] = jnp.broadcast_to(total, shape)
                    state[m, 2, span, :] = mean

            if r == 0:
                block(True)
            else:
                clear = begin >= key_last
                some = begin + half - 1 >= key_begin
                pl.when(clear)(lambda block=block: block(False))
                pl.when(jnp.logical_and(some, jnp.logical_not(clear)))(lambda block=block: block(True))


def attend_kernel(rels, info, query, *refs):
    n = len(rels)
    pieces = refs[:n]
    if rels[0] == 0:
        state = refs[n]
    else:
        state = refs[n + 1]
        state[...] = refs[n][...]
    attend(rels, info[0], query, pieces, state)


def finish_kernel(
    rels, every, info, lambdas, query, pool, tails, gain, weight, scale, held, *refs
):
    n = len(rels)
    pieces, (same, other, state, act) = refs[:n], refs[n:]
    s, t = info[0], info[1]
    low = (s // HB) % 2
    rows = query.shape[0]
    half = rows // 2
    state[...] = held[...]
    attend(rels, s, query, pieces, state)
    w = VALUE_DIM
    head = 2 * t + low
    means = [state[m, 2] / state[m, 1] for m in range(2)]
    differed = means[0] - lambdas[head] * means[1]
    square = jnp.mean(differed * differed, axis=-1, keepdims=True)
    scaled = differed * lax.rsqrt(square + head_floor) * gain[...] * head_scale
    act[:, :w] = scaled.astype(jnp.bfloat16)

    kind = head % 4
    span = lax.shift_left(2, kind)
    base = s - low * HB
    for i in range(2):
        mine = base + i * HB
        before = jnp.zeros((HALO, w), jnp.float32)
        for k, r in enumerate(every):
            for j in range(2):
                hit = (base ^ r) + j * HB == mine - 1
                tail = tails[k * HALO : (k + 1) * HALO, j * w : (j + 1) * w]
                before = jnp.where(hit, tail.astype(jnp.float32), before)
        here = pool[i * half : (i + 1) * half, :].astype(jnp.float32)
        sums = jnp.concatenate([before, here], axis=0)
        picked = sums
        for step in range(4):
            sums = sums + pltpu.roll(sums, 2**step, 0)
            picked = jnp.where(kind == step, sums, picked)
        place = mine * half + lax.broadcasted_iota(jnp.int32, (half, w), 0)
        counts = jnp.minimum(place + 1, span).astype(jnp.float32)
        window = picked[HALO:, :] / counts - here
        mixed = jnp.dot(window.astype(jnp.bfloat16), weight[head], preferred_element_type=jnp.float32)
        mixed = mixed * scale[pl.ds(head, 1), :]
        act[i * half : (i + 1) * half, w:] = mixed.astype(jnp.bfloat16)

    part = half // 4
    for k in range(4):
        at = (low ^ (k // 2)) * half + ((t ^ (k % 2 * Y)) * part)
        near = pl.multiple_of(at, part)
        far = pl.multiple_of((low ^ (k // 2)) * half + (t ^ (k % 2 * Y) ^ C) * part, part)
        same[k * part : (k + 1) * part, :] = act[pl.ds(near, part), :]
        other[k * part : (k + 1) * part, :] = act[pl.ds(far, part), :]


def mix_kernel(rels, info, near, far, near_weight, far_weight, own, *sends):
    s = info[0]
    cols = near_weight.shape[2]
    part = own.shape[0]
    for k, r in enumerate(rels):
        col = 0 if len(rels) == 1 else pl.multiple_of((s ^ r) * cols, cols)
        made = jnp.dot(near[...], near_weight[k], preferred_element_type=jnp.float32)
        made = made + jnp.dot(far[...], far_weight[k], preferred_element_type=jnp.float32)
        own[:, pl.ds(col, cols)] = made[:part, :]
        for j, send in enumerate(sends):
            piece = made[(j + 1) * part : (j + 2) * part, :]
            send[:, pl.ds(col, cols)] = piece.astype(jnp.bfloat16)


def body(sizes, *args):
    (
        tokens,
        norm_gain,
        query_one,
        key_one,
        query_two,
        key_two,
        value_weight,
        pool_weight,
        lambda_head,
        head_gain,
        group_weight,
        pool_scale,
        out_attn,
        out_pool,
    ) = args
    n_s, n_t = sizes
    s, t = lax.axis_index("sp"), lax.axis_index("tp")
    info = jnp.stack([s, t]).astype(jnp.int32)
    rows, feats = tokens.shape
    deep, depth = query_one.shape[0], feats * n_t
    bf16, f32 = jnp.bfloat16, jnp.float32

    def swap(x, s_bits, t_bits, keep=lambda target: True):
        pairs = [
            (a * n_t + b, (a ^ s_bits) * n_t + (b ^ t_bits))
            for a in range(n_s)
            for b in range(n_t)
            if keep(a ^ s_bits)
        ]
        return lax.ppermute(x, ("sp", "tp"), pairs)

    highs = [r for r in range(n_s) if r & (X | HB) == 0]

    def spread(same, other):
        pieces = {0: same, HB: swap(other, HB, 0)}
        for r in highs[1:]:
            pieces[r] = swap(same, r, 0)
            pieces[r | HB] = swap(other, r | HB, 0)
        for r in list(pieces):
            pieces[r | X] = swap(pieces[r], X, 0)
        return pieces

    def shape(*dims, dtype=bf16):
        return jax.ShapeDtypeStruct(dims, dtype)

    w = VALUE_DIM
    same, other = call(
        pack_kernel,
        (shape(deep, 4 * w),) * 2,
        (info, query_one, key_one, query_two, key_two, value_weight, pool_weight),
        name="pack",
    )
    weights = spread(same, other)
    arrived = [tokens, None, swap(tokens, 0, Y), None]
    arrived += [swap(tokens, HB, 0), None, swap(tokens, HB, Y), None]
    for k in range(0, 8, 2):
        arrived[k + 1] = swap(arrived[k], 0, C)
    normed = call(
        norm_kernel,
        shape(2 * rows, depth),
        (info, norm_gain[None, :], *arrived),
        name="norm",
    )

    base = s - (s // HB % 2) * HB
    positions = jnp.concatenate([(base + i * HB) * rows + jnp.arange(rows) for i in range(2)])
    half_dim = HEAD_DIM // 2
    inverse = rope_base ** (-(jnp.arange(half_dim, dtype=f32) * 2.0 / HEAD_DIM))
    angles = positions.astype(f32)[:, None] * inverse[None, :]
    cosine, sine = jnp.cos(angles), jnp.sin(angles)
    cosine = jnp.concatenate([cosine] * 4, axis=1)
    sine = jnp.concatenate([-sine, sine] * 2, axis=1)

    rels = sorted(weights)
    query, keyval, pool = call(
        lambda *refs: project_kernel(rels, *refs),
        (shape(2 * rows, w), shape(2 * rows + HALO, 2 * w), shape(2 * rows, w)),
        (info, normed, cosine, sine, *[weights[r] for r in rels]),
        scratch=[pltpu.VMEM((depth, 4 * w), bf16)],
        name="project",
    )

    def later(r):
        top = 1 << (r.bit_length() - 1)
        return lambda target: top < HB or bool(target & top)

    known = {0: keyval}
    for r in highs[1:]:
        known[r] = swap(keyval, r, 0, later(r))
    for r in list(known):
        known[r | X] = swap(known[r], X, 0, later(r | X))
    every = sorted(known)
    state = None
    state_shape = shape(2, 3, 2 * rows, w, dtype=f32)
    for k in range(0, len(every) - 2, 2):
        pair = every[k : k + 2]
        extra = () if state is None else (state,)
        state = call(
            lambda *refs, pair=pair: attend_kernel(pair, *refs),
            state_shape,
            (info, query, *[known[r] for r in pair], *extra),
            name="attend",
        )
    tails = jnp.concatenate([known[r][2 * rows :] for r in every], axis=0)
    part = rows // n_t
    pair = every[-2:]
    near, far = pl.pallas_call(
        lambda *refs: finish_kernel(pair, every, *refs),
        out_shape=(shape(4 * part, 2 * w),) * 2,
        in_specs=[SMEM, SMEM] + [VMEM] * 9,
        out_specs=(VMEM, VMEM),
        scratch_shapes=[pltpu.VMEM(state_shape.shape, f32), pltpu.VMEM((2 * rows, 2 * w), bf16)],
        name="finish",
        compiler_params=pltpu.CompilerParams(vmem_limit_bytes=48 * 1024 * 1024),
    )(
        info,
        lambda_head,
        query,
        pool,
        tails,
        head_gain[None, :],
        group_weight,
        pool_scale.reshape(-1, w),
        state,
        *[known[r] for r in pair],
    )
    far = swap(far, 0, C)

    cols = out_attn.shape[1]
    same, other = call(
        pack_out_kernel, (shape(2 * w, cols),) * 2, (info, out_attn, out_pool), name="pack_out"
    )
    outs = spread(same, other)
    rels = sorted(outs)
    near_weight = jnp.stack([outs[r] for r in rels])
    if cols % w:
        order = jnp.arange(n_s) ^ s
        near_weight = jnp.take(near_weight, order, axis=0).transpose(1, 0, 2)
        near_weight = near_weight.reshape(1, 2 * w, n_s * cols)
        rels = [0]
    far_weight = swap(near_weight, 0, C)
    own, *sends = call(
        lambda *refs: mix_kernel(rels, *refs),
        (shape(part, n_s * cols, dtype=f32),) + (shape(part, n_s * cols),) * 3,
        (info, near, far, near_weight, far_weight),
        name="mix",
    )
    got = [swap(sends[0], 0, Y), swap(sends[1], HB, 0), swap(sends[2], HB, Y)]
    return (own + got[0] + got[1] + got[2]).astype(bf16)


def solution(mesh):
    sizes = (mesh.shape["sp"], mesh.shape["tp"])
    split = P("sp", "tp")
    in_specs = (split, P()) + (split,) * 6 + (P(),) * 4 + (P("tp", "sp"),) * 2
    return jax.shard_map(
        lambda *args: body(sizes, *args),
        mesh=mesh,
        in_specs=in_specs,
        out_specs=P(("sp", "tp"), None),
        check_vma=False,
    )
```
